256 devices in a mesh: grp: 2 (over y), sp: 16 (over z), dp: 8 (over x, core).
Axes of the slice: x: 4, y: 2, z: 16, core: 2. Of those that a mesh axis runs over, the one named last changes fastest.
The devices are a block of a 4x16x16 slice.
Arguments:
- activations: bfloat16 [16, 8192, 2048], P(('grp', 'dp'), 'sp'), parts along dimension 0, may hold values from -6 to 6
- value_weight: bfloat16 [2048, 1024], P('sp', 'dp'), may hold values from -0.125 to 0.125
- gate_weight: bfloat16 [2048, 1024], P('sp', 'dp'), may hold values from -0.125 to 0.125
- conv_taps: float32 [31, 1024], replicated, may hold values from -4 to 4
- conv_bias: float32 [1024], replicated, may hold values from -3 to 3
- norm_gain: float32 [1024], replicated, may hold values from 0.1 to 1.9
- norm_bias: float32 [1024], replicated, may hold values from -3 to 3
- out_weight: bfloat16 [1024, 2048], P('sp', 'dp'), may hold values from -0.1875 to 0.1875
Outputs:
- mixed_out: bfloat16 [16, 8192, 2048], P(('grp', 'dp'), 'sp'), parts along dimension 0
The draws below stay inside these ranges and needn't reach their ends.
There are 2 independent parts, one for each index of `grp`. The reference program is written for one: setup_inputs(seed, part) draws one part's arguments, and reference() takes and returns one part's arrays. A program takes and returns all parts, laid end to end along the dimension named above; an argument that names none is the same for every part. Nothing has to cross between parts.
All inputs are finite; a program needn't handle non-finite values.
Results may differ from the reference program's by a relative error of at most 0.013.
Values may be sent and summed in bfloat16 or wider, within the bound.
No kernel may reach another device: no remote copies, remote signals or barrier semaphores. Data moves between devices by JAX's collectives and lax.ppermute only.
A program may use at most 64 MiB of HBM per device.

```python
import jax
import jax.numpy as jnp
from jax import lax

D = 2048
C = 1024
KW = 31
LEN = 8192
SEQS = 8


def draw_conv_taps(key, part):
    key_base = jax.random.fold_in(key, 11)
    key_level = jax.random.fold_in(key, 12)
    blocks = C // 16
    levels = jax.random.uniform(key_level, (blocks,), jnp.float32, -1.2, 1.2)
    scales = jnp.repeat(jnp.exp(levels), 16)
    base = jnp.clip(jax.random.normal(key_base, (KW, C), jnp.float32), -3.0, 3.0)
    return jnp.clip(base * scales[None, :] * KW ** (-0.5), -4.0, 4.0)


def level_of(own_key, dims, shards, low, top_value):
    def one(dim, parts):
        heights = jax.random.uniform(jax.random.fold_in(jax.random.fold_in(own_key, 6), dim), (parts,), jnp.float32, low / len(shards), top_value / len(shards))
        return jnp.repeat(jnp.exp(heights), dims[dim] // parts).reshape((-1,) + (1,) * (len(dims) - dim - 1))

    factor_of = one(*shards[0])
    for cut in shards[1:]:
        factor_of = factor_of * one(*cut)
    return factor_of


def centred(rng, extent, scale, bound, pieces=(), kind=jnp.bfloat16):
    factor_of = level_of(rng, extent, pieces, -0.22, 0.18) if pieces else 1.0
    array = jax.random.normal(rng, extent, jnp.float32) * scale * factor_of
    return jnp.minimum(jnp.maximum(array, -bound), bound).astype(kind)


def setup_inputs(seed: int = 0, part: int = 0) -> dict:
    keys = jax.random.split(jax.random.key(seed), 9)
    own_keys = jax.random.split(jax.random.fold_in(keys[8], part), 9)
    return {
        "activations": centred(own_keys[0], (SEQS, LEN, D), 1.0, 6.0, ((0, 8), (1, 16))),
        "value_weight": centred(keys[1], (D, C), D ** -0.5, 0.125, ((0, 16), (1, 8))),
        "gate_weight": centred(keys[2], (D, C), D ** -0.5, 0.125, ((0, 16), (1, 8))),
        "conv_taps": draw_conv_taps(jax.random.fold_in(keys[8], 71), part),
        "conv_bias": centred(keys[4], (C,), 0.5, 3.0, (), jnp.float32),
        "norm_gain": jnp.clip(1.0 + 0.18 * jax.random.normal(keys[5], (C,), jnp.float32), 0.1, 1.9),
        "norm_bias": centred(keys[6], (C,), 0.5, 3.0, (), jnp.float32),
        "out_weight": centred(keys[7], (C, D), C ** -0.5, 0.1875, ((0, 16), (1, 8))),
    }


epsilon = 1e-05

def one_sequence(rows, value_weight, gate_weight, conv_taps, conv_bias, norm_gain, norm_bias, out_weight):
    values = jnp.dot(rows, value_weight, preferred_element_type=jnp.float32).astype(jnp.bfloat16)
    gates = jnp.dot(rows, gate_weight, preferred_element_type=jnp.float32).astype(jnp.bfloat16)
    gated_rows = (values.astype(jnp.float32) * jax.nn.sigmoid(gates.astype(jnp.float32))).astype(jnp.bfloat16)
    padded = jnp.pad(gated_rows.astype(jnp.float32), ((KW - 1, 0), (0, 0)))
    length = rows.shape[0]
    conv_sum = jnp.zeros((length, C), jnp.float32) + conv_bias[None, :]
    for tap_index in range(KW):
        conv_sum = conv_sum + conv_taps[tap_index][None, :] * padded[tap_index:tap_index + length]
    mean_row = lax.optimization_barrier(jnp.mean(conv_sum, axis=-1, keepdims=True))
    centered = conv_sum - mean_row
    spread = lax.optimization_barrier(jnp.mean(centered * centered, axis=-1, keepdims=True))
    normed = centered * lax.rsqrt(spread + epsilon) * norm_gain[None, :] + norm_bias[None, :]
    swished = jax.nn.silu(normed).astype(jnp.bfloat16)
    return jnp.dot(swished, out_weight, preferred_element_type=jnp.float32).astype(jnp.bfloat16)

def reference(activations, value_weight, gate_weight, conv_taps, conv_bias, norm_gain, norm_bias, out_weight):

    def single(rows):
        return one_sequence(rows, value_weight, gate_weight, conv_taps, conv_bias, norm_gain, norm_bias, out_weight)
    return lax.map(single, activations)
```

```python
import functools

import jax
import jax.numpy as jnp
from jax import lax
from jax.experimental import pallas as pl
from jax.experimental.pallas import tpu as pltpu
from jax.sharding import PartitionSpec as P

epsilon = 1e-05
SCALE = 2.0**18
HALO = 32
ROWS = 64


def whole(space=pltpu.VMEM):
    return pl.BlockSpec(memory_space=space)


def conv_kernel(counts, index_ref, taps_ref, bias_ref, rows_ref, *refs):
    n_pieces = sum(counts)
    pieces, outs, gated = refs[:n_pieces], refs[n_pieces:-1], refs[-1]
    tok_rows = outs[0].shape[0]
    width = outs[0].shape[1]
    kernel_len = taps_ref.shape[0]
    first = 0
    for k, count in enumerate(counts):
        both = None
        at = 0
        for piece in pieces[first : first + count]:
            depth = piece.shape[0]
            part = jnp.dot(rows_ref[:, at : at + depth], piece[...], preferred_element_type=jnp.float32)
            both = part if both is None else both + part
            at += depth
        first += count
        value = both[:, :width].astype(jnp.bfloat16).astype(jnp.float32)
        gate = both[:, width:].astype(jnp.bfloat16).astype(jnp.float32)
        gated[...] = (value * jax.nn.sigmoid(gate)).astype(jnp.bfloat16).astype(jnp.float32)
        lane = pl.multiple_of(index_ref[k] * width, width)
        out = outs[k]
        bias = bias_ref[:, pl.ds(lane, width)]
        taps = [taps_ref[j : j + 1, pl.ds(lane, width)] for j in range(kernel_len)]

        def tile(i, carry, out=out, bias=bias, taps=taps):
            start = pl.multiple_of(i * ROWS, ROWS)
            total = jnp.broadcast_to(bias, (ROWS, width))
            for j in range(kernel_len):
                total = total + taps[j] * gated[pl.ds(start + (HALO - kernel_len + 1 + j), ROWS), :]
            out[pl.ds(start, ROWS), :] = total
            return carry

        lax.fori_loop(0, tok_rows // ROWS, tile, 0)


def conv_blocks(rows, blocks, indices, taps, bias):
    tok_rows = rows.shape[0] - HALO
    width = blocks[0][0].shape[1] // 2
    counts = tuple(len(b) for b in blocks)
    pieces = [p for b in blocks for p in b]
    flops = 2 * rows.shape[0] * rows.shape[1] * 2 * width * len(blocks)
    return pl.pallas_call(
        functools.partial(conv_kernel, counts),
        out_shape=[jax.ShapeDtypeStruct((tok_rows, width), jnp.float32) for _ in blocks],
        in_specs=[whole(pltpu.SMEM)] + [whole()] * (3 + len(pieces)),
        out_specs=[whole()] * len(blocks),
        scratch_shapes=[pltpu.VMEM((rows.shape[0], width), jnp.float32)],
        cost_estimate=pl.CostEstimate(flops=flops, bytes_accessed=rows.size * 2, transcendentals=0),
        name="conv_blocks",
    )(jnp.stack(indices).astype(jnp.int32), taps, bias, rows, *pieces)


def norm_kernel(n_blocks, index_ref, gain_ref, shift_ref, *refs):
    blocks, out = refs[:n_blocks], refs[n_blocks]
    tok_rows, width = blocks[0].shape
    channels = n_blocks * width

    def tile(i, carry):
        at = pl.ds(pl.multiple_of(i * ROWS, ROWS), ROWS)
        values = [b[at, :] for b in blocks]
        mean = jnp.sum(sum(values[1:], values[0]), axis=-1, keepdims=True) / channels
        values = [v - mean for v in values]
        squares = [v * v for v in values]
        spread = jnp.sum(sum(squares[1:], squares[0]), axis=-1, keepdims=True) / channels
        scale = lax.rsqrt(spread + epsilon)
        for k, v in enumerate(values):
            lane = pl.multiple_of(index_ref[k] * width, width)
            normed = v * scale * gain_ref[:, pl.ds(lane, width)] + shift_ref[:, pl.ds(lane, width)]
            out[at, pl.ds(lane, width)] = jax.nn.silu(normed).astype(jnp.bfloat16)
        return carry

    lax.fori_loop(0, tok_rows // ROWS, tile, 0)


def norm_blocks(blocks, indices, gain, shift):
    tok_rows, width = blocks[0].shape
    return pl.pallas_call(
        functools.partial(norm_kernel, len(blocks)),
        out_shape=jax.ShapeDtypeStruct((tok_rows, width * len(blocks)), jnp.bfloat16),
        in_specs=[whole(pltpu.SMEM)] + [whole()] * (2 + len(blocks)),
        out_specs=whole(),
        cost_estimate=pl.CostEstimate(flops=tok_rows * width * 1000, bytes_accessed=tok_rows * width * 32, transcendentals=0),
        name="norm_blocks",
    )(jnp.stack(indices).astype(jnp.int32), gain, shift, *blocks)


def out_kernel(counts, index_ref, rows_ref, *refs):
    n_pieces, n_blocks = sum(counts), len(counts)
    pieces = refs[:n_pieces]
    out, held, sems = refs[-3:]
    first = 0
    copies = []
    for k, count in enumerate(counts):
        total = None
        at = 0
        for piece in pieces[first : first + count]:
            depth, width = piece.shape
            part = jnp.dot(rows_ref[:, at : at + depth], piece[...], preferred_element_type=jnp.float32)
            total = part if total is None else total + part
            at += depth
        first += count
        held[k] = total.astype(jnp.bfloat16)
        lane = pl.multiple_of(index_ref[k] * width, width)
        copies.append(pltpu.make_async_copy(held.at[k], out.at[:, pl.ds(lane, width)], sems.at[k]))
        copies[-1].start()
    for copy in copies:
        copy.wait()


def out_blocks(rows, blocks, indices, n_blocks, base=None):
    width = blocks[0][0].shape[1]
    counts = tuple(len(b) for b in blocks)
    pieces = [p for b in blocks for p in b]
    more = [] if base is None else [base]
    return pl.pallas_call(
        functools.partial(out_kernel, counts),
        out_shape=jax.ShapeDtypeStruct((rows.shape[0], width * n_blocks), jnp.bfloat16),
        in_specs=[whole(pltpu.SMEM)] + [whole()] * (1 + len(pieces)) + [whole(pl.ANY)] * len(more),
        out_specs=whole(pl.ANY),
        scratch_shapes=[
            pltpu.VMEM((len(blocks), rows.shape[0], width), jnp.bfloat16),
            pltpu.SemaphoreType.DMA((len(blocks),)),
        ],
        input_output_aliases={2 + len(pieces): 0} if more else {},
        cost_estimate=pl.CostEstimate(flops=2 * rows.size * width * len(blocks), bytes_accessed=rows.size * 6, transcendentals=0),
        name="out_blocks",
    )(jnp.stack(indices).astype(jnp.int32), rows, *pieces, *more)


def local(activations, value_weight, gate_weight, conv_taps, conv_bias, norm_gain, norm_bias, out_weight):
    tokens = activations[0]
    n_sp, n_dp = lax.axis_size("sp"), lax.axis_size("dp")
    me = lax.axis_index("dp")

    def from_next(a):
        return lax.ppermute(a, "dp", [(i, (i - 2) % n_dp) for i in range(n_dp)])

    def from_last(a):
        return lax.ppermute(a, "dp", [(i, (i + 2) % n_dp) for i in range(n_dp)])

    def from_core(a):
        return lax.ppermute(a, "dp", [(i, i ^ 1) for i in range(n_dp)])

    halo = lax.ppermute(tokens[-HALO:], "sp", [(i, i + 1) for i in range(n_sp - 1)])

    depth = value_weight.shape[0]
    packed = jnp.concatenate([jnp.concatenate([value_weight, gate_weight], axis=1), out_weight], axis=0)
    packed = (packed.astype(jnp.float32) * SCALE).astype(jnp.float16)
    packed = lax.all_gather(packed, "sp", axis=0)
    packed = (packed.astype(jnp.float32) * (1.0 / SCALE)).astype(jnp.bfloat16)
    width = packed.shape[-1]
    v_own = packed[:, :depth].reshape(-1, width)
    o_own = packed[:, depth:].reshape(-1, width)
    halo, _ = lax.optimization_barrier((halo, v_own))
    rows = jnp.concatenate([halo, tokens], axis=0)

    hold = lax.optimization_barrier
    half = v_own.shape[0] // 2
    o_half = o_own.shape[0] // 2
    bias, gain, shift = conv_bias[None, :], norm_gain[None, :], norm_bias[None, :]
    nxt, last, far = (me + 2) % n_dp, (me - 2) % n_dp, (me + 4) % n_dp
    order = [me, me ^ 1, nxt, nxt ^ 1, last, last ^ 1, far, far ^ 1]

    v_next, v_last = from_next(v_own), from_last(v_own)
    conv_a = conv_blocks(rows, [[v_own], [from_core(v_own)]], order[:2], conv_taps, bias)
    v_next, v_last, conv_a = hold((v_next, v_last, conv_a))
    far_a, far_b = from_next(v_next[:half]), from_last(v_last[half:])
    conv_b = conv_blocks(
        rows, [[v_next], [from_core(v_next)], [v_last], [from_core(v_last)]], order[2:6], conv_taps, bias
    )
    far_a, far_b, o_own, conv_b = hold((far_a, far_b, o_own, conv_b))
    o_next, o_last = from_next(o_own), from_last(o_own)
    conv_c = conv_blocks(rows, [[far_a, far_b], [from_core(far_a), from_core(far_b)]], order[6:], conv_taps, bias)
    swished = norm_blocks(conv_a + conv_b + conv_c, order, gain, shift)
    o_next, o_last, swished = hold((o_next, o_last, swished))
    o_far_a, o_far_b = from_next(o_next[:o_half]), from_last(o_last[o_half:])
    result = out_blocks(
        swished,
        [[o_own], [from_core(o_own)], [o_next], [from_core(o_next)], [o_last], [from_core(o_last)]],
        order[:6],
        n_dp,
    )
    o_far_a, o_far_b, result = hold((o_far_a, o_far_b, result))
    result = out_blocks(
        swished, [[o_far_a, o_far_b], [from_core(o_far_a), from_core(o_far_b)]], order[6:], n_dp, result
    )
    return result[None]


def solution(mesh):
    in_specs = (
        P(("grp", "dp"), "sp", None),
        P("sp", "dp"),
        P("sp", "dp"),
        P(),
        P(),
        P(),
        P(),
        P("sp", "dp"),
    )
    out_specs = P(("grp", "dp"), "sp", None)
    return jax.shard_map(local, mesh=mesh, in_specs=in_specs, out_specs=out_specs, check_vma=False)
```

```python
import functools

import jax
import jax.numpy as jnp
from jax import lax
from jax.experimental import pallas as pl
from jax.experimental.pallas import tpu as pltpu
from jax.sharding import PartitionSpec as P


epsilon = 1e-05
SCALE = 2.0**18
HALO = 32
ROWS = 64


def whole(space=pltpu.VMEM):
    return pl.BlockSpec(memory_space=space)


def convolve(gated, taps, bias, store, tok_rows):
    kernel_len = taps.shape[0]
    lead = HALO - kernel_len + 1
    for start in range(0, tok_rows, ROWS):
        n_tiles = ROWS // 8
        totals = [bias] * n_tiles
        for shift in range(8):
            near = [(q, 8 * q + shift - lead) for q in range((HALO + 8) // 8)]
            near = [(q, j) for q, j in near if 0 <= j < kernel_len]
            weights = [(q, taps[j]) for q, j in near]
            for m in range(n_tiles + near[-1][0]):
                users = [(m - q, w) for q, w in weights if 0 <= m - q < n_tiles]
                if not users:
                    continue
                row = gated[pl.ds(start + 8 * m + shift, 8), :]
                for tile, w in users:
                    totals[tile] = totals[tile] + w * row
        for tile, total in enumerate(totals):
            store(start + 8 * tile, total)


def conv_kernel(counts, first, n_done, index_ref, taps_ref, bias_ref, *refs):
    n_pieces, n_blocks = sum(counts), len(counts)
    norm = n_done > 0
    if norm:
        (gain_ref, shift_ref), refs = refs[:2], refs[2:]
    rows_hbm, pieces, refs = refs[0], refs[1 : 1 + n_pieces], refs[1 + n_pieces :]
    done, refs = refs[:n_done], refs[n_done:]
    n_outs = 1 if norm else n_blocks
    outs, refs = refs[:n_outs], refs[n_outs:]
    rows, held, gated, taps_held, sems, conv = refs
    tok_rows, width = rows.shape[0] - HALO, gated.shape[-1]
    kernel_len = taps_ref.shape[0]

    copies = [pltpu.make_async_copy(rows_hbm, rows, sems.at[0])]
    at = 0
    for k, count in enumerate(counts):
        depth = 0
        for _ in range(count):
            size = pieces[at].shape[0]
            copies.append(pltpu.make_async_copy(pieces[at], held.at[k, pl.ds(depth, size), :], sems.at[1 + at]))
            depth += size
            at += 1
    for k in range(n_done):
        copies.append(pltpu.make_async_copy(done[k], conv.at[k], sems.at[1 + n_pieces + k]))
    for copy in copies:
        copy.start()

    def lane_of(k):
        return pl.multiple_of(index_ref[first + k] * width, width)

    def project(k):
        at = 1 + sum(counts[:k])
        for copy in copies[at : at + counts[k]]:
            copy.wait()
        return jnp.dot(rows[...], held[k], preferred_element_type=jnp.float32)

    def gate(k, both):
        value = both[:, :width].astype(jnp.bfloat16).astype(jnp.float32)
        gates = both[:, width:].astype(jnp.bfloat16).astype(jnp.float32)
        gated[k % 2] = (value * jax.nn.sigmoid(gates)).astype(jnp.bfloat16).astype(jnp.float32)
        for j in range(kernel_len):
            taps_held[k % 2, j] = jnp.broadcast_to(taps_ref[j : j + 1, pl.ds(lane_of(k), width)], (8, width))

    def filter_block(k):
        bias = jnp.broadcast_to(bias_ref[:, pl.ds(lane_of(k), width)], (8, width))

        def store(at, value):
            if norm:
                conv[n_done + k, pl.ds(at, 8), :] = value
            else:
                outs[k][pl.ds(at, 8), :] = value

        convolve(gated.at[k % 2], taps_held.at[k % 2], bias, store, tok_rows)

    copies[0].wait()
    gate(0, project(0))
    for k in range(1, n_blocks):
        both = project(k)
        filter_block(k - 1)
        gate(k, both)
    filter_block(n_blocks - 1)
    for copy in copies[1 + n_pieces :]:
        copy.wait()
    if not norm:
        return

    out = outs[0]
    total = n_done + n_blocks
    lanes = [pl.multiple_of(index_ref[k] * width, width) for k in range(total)]

    def tile(i, carry):
        at = pl.ds(pl.multiple_of(i * 16, 16), 16)
        values = [conv[k, at, :] for k in range(total)]
        mean = jnp.sum(sum(values[1:], values[0]), axis=-1, keepdims=True) / (total * width)
        values = [v - mean for v in values]
        squares = [v * v for v in values]
        spread = jnp.sum(sum(squares[1:], squares[0]), axis=-1, keepdims=True) / (total * width)
        scale = lax.rsqrt(spread + epsilon)
        for v, lane in zip(values, lanes):
            normed = v * scale * gain_ref[:, pl.ds(lane, width)] + shift_ref[:, pl.ds(lane, width)]
            out[at, pl.ds(lane, width)] = jax.nn.silu(normed).astype(jnp.bfloat16)
        return carry

    lax.fori_loop(0, tok_rows // 16, tile, 0, unroll=4)


def conv_blocks(rows, blocks, index, first, taps, bias, done=(), gain=None, shift=None):
    tok_rows = rows.shape[0] - HALO
    width = blocks[0][0].shape[1] // 2
    counts = tuple(len(b) for b in blocks)
    pieces = [p for b in blocks for p in b]
    n_blocks, n_done = len(blocks), len(done)
    norm = n_done > 0
    if norm:
        outs = [jax.ShapeDtypeStruct((tok_rows, width * (n_done + n_blocks)), jnp.bfloat16)]
    else:
        outs = [jax.ShapeDtypeStruct((tok_rows, width), jnp.float32) for _ in blocks]
    flops = 2 * rows.shape[0] * rows.shape[1] * 2 * width * n_blocks
    return pl.pallas_call(
        functools.partial(conv_kernel, counts, first, n_done),
        out_shape=outs,
        in_specs=[whole(pltpu.SMEM)]
        + [whole()] * (4 if norm else 2)
        + [whole(pl.ANY)] * (1 + len(pieces) + n_done),
        out_specs=[whole()] * len(outs),
        scratch_shapes=[
            pltpu.VMEM(rows.shape, rows.dtype),
            pltpu.VMEM((n_blocks, rows.shape[1], 2 * width), rows.dtype),
            pltpu.VMEM((2, rows.shape[0], width), jnp.float32),
            pltpu.VMEM((2, taps.shape[0], 8, width), jnp.float32),
            pltpu.SemaphoreType.DMA((1 + len(pieces) + n_done,)),
            pltpu.VMEM((n_done + n_blocks, tok_rows, width) if norm else (1, 8, width), jnp.float32),
        ],
        cost_estimate=pl.CostEstimate(flops=flops, bytes_accessed=rows.size * 2, transcendentals=0),
        name="conv_norm" if norm else "conv_blocks",
    )(index, taps, bias, *((gain, shift) if norm else ()), rows, *pieces, *done)


def out_kernel(counts, first, index_ref, rows_ref, *refs):
    n_pieces = sum(counts)
    pieces = refs[:n_pieces]
    out, held, sems = refs[-3:]
    begin = 0
    copies = []
    for k, count in enumerate(counts):
        total = None
        at = 0
        for piece in pieces[begin : begin + count]:
            depth, width = piece.shape
            part = jnp.dot(rows_ref[:, at : at + depth], piece[...], preferred_element_type=jnp.float32)
            total = part if total is None else total + part
            at += depth
        begin += count
        held[k] = total.astype(jnp.bfloat16)
        lane = pl.multiple_of(index_ref[first + k] * width, width)
        copies.append(pltpu.make_async_copy(held.at[k], out.at[:, pl.ds(lane, width)], sems.at[k]))
        copies[-1].start()
    for copy in copies:
        copy.wait()


def out_blocks(rows, blocks, index, first, n_blocks, base=None):
    width = blocks[0][0].shape[1]
    counts = tuple(len(b) for b in blocks)
    pieces = [p for b in blocks for p in b]
    more = [] if base is None else [base]
    return pl.pallas_call(
        functools.partial(out_kernel, counts, first),
        out_shape=jax.ShapeDtypeStruct((rows.shape[0], width * n_blocks), jnp.bfloat16),
        in_specs=[whole(pltpu.SMEM)] + [whole()] * (1 + len(pieces)) + [whole(pl.ANY)] * len(more),
        out_specs=whole(pl.ANY),
        scratch_shapes=[
            pltpu.VMEM((len(blocks), rows.shape[0], width), jnp.bfloat16),
            pltpu.SemaphoreType.DMA((len(blocks),)),
        ],
        input_output_aliases={2 + len(pieces): 0} if more else {},
        cost_estimate=pl.CostEstimate(flops=2 * rows.size * width * len(blocks), bytes_accessed=rows.size * 6, transcendentals=0),
        name="out_blocks",
    )(index, rows, *pieces, *more)


def work(activations, value_weight, gate_weight, conv_taps, conv_bias, norm_gain, norm_bias, out_weight):
    tokens = activations[0]
    n_sp, n_dp = lax.axis_size("sp"), lax.axis_size("dp")
    me = lax.axis_index("dp")

    def from_next(a):
        return lax.ppermute(a, "dp", [(i, (i - 2) % n_dp) for i in range(n_dp)])

    def from_last(a):
        return lax.ppermute(a, "dp", [(i, (i + 2) % n_dp) for i in range(n_dp)])

    def from_core(a):
        return lax.ppermute(a, "dp", [(i, i ^ 1) for i in range(n_dp)])

    halo = lax.ppermute(tokens[-HALO:], "sp", [(i, i + 1) for i in range(n_sp - 1)])

    hold = lax.optimization_barrier
    depth = value_weight.shape[0]
    packed = jnp.concatenate([jnp.concatenate([value_weight, gate_weight], axis=1), out_weight], axis=0)
    packed = (packed.astype(jnp.float32) * SCALE).astype(jnp.float16)
    packed, halo = hold((packed, halo))
    packed = lax.all_gather(packed, "sp", axis=0)
    packed = (packed.astype(jnp.float32) * (1.0 / SCALE)).astype(jnp.bfloat16)
    width = packed.shape[-1]
    upper = packed[: n_sp // 2, :depth].reshape(-1, width)
    lower = packed[n_sp // 2 :, :depth].reshape(-1, width)
    o_own = packed[:, depth:].reshape(-1, width)
    o_half = o_own.shape[0] // 2
    bias, gain, shift = conv_bias[None, :], norm_gain[None, :], norm_bias[None, :]
    place = jnp.arange(n_dp, dtype=jnp.int32)
    chip = place // 2
    step = jnp.where(chip == 2, -2, jnp.where(chip == 3, 4, 2 * chip))
    index = ((me + step) % n_dp) ^ (place % 2)

    next_a, last_b = from_next(upper), from_last(lower)
    next_b, last_a = from_next(lower), from_last(upper)
    rows = jnp.concatenate([halo, tokens], axis=0)
    own_swap = [from_core(upper), from_core(lower)]
    conv_a = conv_blocks(rows, [[upper, lower], own_swap], index, 0, conv_taps, bias)
    next_a, last_b, conv_a = hold((next_a, last_b, conv_a))
    far_a, far_b = from_next(next_a), from_last(last_b)
    next_b, last_a, o_send = hold((next_b, last_a, o_own))
    o_next, o_last = from_next(o_send), from_last(o_send)
    o_swap = from_core(o_send)
    swaps = [[from_core(next_a), from_core(next_b)], [from_core(last_a), from_core(last_b)]]
    conv_b = conv_blocks(
        rows, [[next_a, next_b], swaps[0], [last_a, last_b], swaps[1]], index, 2, conv_taps, bias
    )
    far_a, far_b, conv_b = hold((far_a, far_b, conv_b))
    (swished,) = conv_blocks(
        rows, [[far_a, far_b], [from_core(far_a), from_core(far_b)]], index, 6, conv_taps, bias,
        conv_a + conv_b, gain, shift,
    )
    o_next, o_last, swished = hold((o_next, o_last, swished))
    o_far_a, o_far_b = from_next(o_next[:o_half]), from_last(o_last[o_half:])
    o_swaps = from_core(o_next), from_core(o_last)
    result = out_blocks(
        swished, [[o_send], [o_swap], [o_next], [o_swaps[0]], [o_last], [o_swaps[1]]], index, 0, n_dp
    )
    o_far_a, o_far_b, result = hold((o_far_a, o_far_b, result))
    result = out_blocks(
        swished, [[o_far_a, o_far_b], [from_core(o_far_a), from_core(o_far_b)]], index, 6, n_dp, result
    )
    return result[None]


def solution(mesh):
    in_specs = (
        P(("grp", "dp"), "sp", None),
        P("sp", "dp"),
        P("sp", "dp"),
        P(),
        P(),
        P(),
        P(),
        P("sp", "dp"),
    )
    out_specs = P(("grp", "dp"), "sp", None)
    return jax.shard_map(work, mesh=mesh, in_specs=in_specs, out_specs=out_specs, check_vma=False)
```

```python
import functools

import jax
import jax.numpy as jnp
from jax import lax
from jax.experimental import pallas as pl
from jax.experimental.pallas import tpu as pltpu
from jax.sharding import PartitionSpec as P


epsilon = 1e-05
SCALE = 2.0**18
HALO = 32
ROWS = 64
VMEM_LIMIT = 16 * 2**20


def whole(space=pltpu.VMEM):
    return pl.BlockSpec(memory_space=space)


def near(a):
    return pltpu.with_memory_space_constraint(a, pltpu.VMEM)


def convolve(gated, taps, bias, store, tok_rows):
    kernel_len = taps.shape[0]
    lead = HALO - kernel_len + 1
    for start in range(0, tok_rows, ROWS):
        n_tiles = ROWS // 8
        totals = [bias] * n_tiles
        for shift in range(8):
            near = [(q, 8 * q + shift - lead) for q in range((HALO + 8) // 8)]
            near = [(q, j) for q, j in near if 0 <= j < kernel_len]
            weights = [(q, taps[j]) for q, j in near]
            for m in range(n_tiles + near[-1][0]):
                users = [(m - q, w) for q, w in weights if 0 <= m - q < n_tiles]
                if not users:
                    continue
                row = gated[pl.ds(start + 8 * m + shift, 8), :]
                for tile, w in users:
                    totals[tile] = totals[tile] + w * row
        for tile, total in enumerate(totals):
            store(start + 8 * tile, total)


def conv_kernel(counts, first, n_done, index_ref, taps_ref, bias_ref, *refs):
    n_pieces, n_blocks = sum(counts), len(counts)
    norm = n_done > 0
    if norm:
        (gain_ref, shift_ref), refs = refs[:2], refs[2:]
    rows, pieces, refs = refs[0], refs[1 : 1 + n_pieces], refs[1 + n_pieces :]
    done, refs = refs[:n_done], refs[n_done:]
    n_outs = 1 if norm else n_blocks
    outs, refs = refs[:n_outs], refs[n_outs:]
    gated, taps_held, conv = refs
    tok_rows, width = rows.shape[0] - HALO, gated.shape[-1]
    kernel_len = taps_ref.shape[0]

    def lane_of(k):
        return pl.multiple_of(index_ref[first + k] * width, width)

    def project(k):
        at, total = 0, None
        for piece in pieces[sum(counts[:k]) : sum(counts[: k + 1])]:
            size = piece.shape[0]
            part = jnp.dot(rows[:, at : at + size], piece[...], preferred_element_type=jnp.float32)
            total = part if total is None else total + part
            at += size
        return total

    def gate(k, both):
        value = both[:, :width].astype(jnp.bfloat16).astype(jnp.float32)
        gates = both[:, width:].astype(jnp.bfloat16).astype(jnp.float32)
        gated[k % 2] = (value * jax.nn.sigmoid(gates)).astype(jnp.bfloat16).astype(jnp.float32)
        for j in range(kernel_len):
            taps_held[k % 2, j] = jnp.broadcast_to(taps_ref[j : j + 1, pl.ds(lane_of(k), width)], (8, width))

    def filter_block(k):
        bias = jnp.broadcast_to(bias_ref[:, pl.ds(lane_of(k), width)], (8, width))

        def store(at, value):
            if norm:
                conv[k, pl.ds(at, 8), :] = value
            else:
                outs[k][pl.ds(at, 8), :] = value

        convolve(gated.at[k % 2], taps_held.at[k % 2], bias, store, tok_rows)

    gate(0, project(0))
    for k in range(1, n_blocks):
        both = project(k)
        filter_block(k - 1)
        gate(k, both)
    filter_block(n_blocks - 1)
    if not norm:
        return

    out = outs[0]
    total = n_done + n_blocks
    lanes = [pl.multiple_of(index_ref[k] * width, width) for k in range(total)]

    def tile(i, carry):
        at = pl.ds(pl.multiple_of(i * 16, 16), 16)
        values = [d[at, :] for d in done] + [conv[k, at, :] for k in range(n_blocks)]
        mean = jnp.sum(sum(values[1:], values[0]), axis=-1, keepdims=True) / (total * width)
        values = [v - mean for v in values]
        squares = [v * v for v in values]
        spread = jnp.sum(sum(squares[1:], squares[0]), axis=-1, keepdims=True) / (total * width)
        scale = lax.rsqrt(spread + epsilon)
        for v, lane in zip(values, lanes):
            normed = v * scale * gain_ref[:, pl.ds(lane, width)] + shift_ref[:, pl.ds(lane, width)]
            out[at, pl.ds(lane, width)] = jax.nn.silu(normed).astype(jnp.bfloat16)
        return carry

    lax.fori_loop(0, tok_rows // 16, tile, 0, unroll=4)


def conv_blocks(rows, blocks, index, first, taps, bias, done=(), gain=None, shift=None):
    tok_rows = rows.shape[0] - HALO
    width = blocks[0][0].shape[1] // 2
    counts = tuple(len(b) for b in blocks)
    pieces = [p for b in blocks for p in b]
    n_blocks, n_done = len(blocks), len(done)
    norm = n_done > 0
    if norm:
        outs = [pltpu.VMEM((tok_rows, width * (n_done + n_blocks)), jnp.bfloat16)]
    else:
        outs = [pltpu.VMEM((tok_rows, width), jnp.float32) for _ in blocks]
    flops = 2 * rows.shape[0] * rows.shape[1] * 2 * width * n_blocks
    return pl.pallas_call(
        functools.partial(conv_kernel, counts, first, n_done),
        out_shape=outs,
        in_specs=[whole(pltpu.SMEM)]
        + [whole()] * (4 if norm else 2)
        + [whole()] * (1 + len(pieces) + n_done),
        out_specs=[whole()] * len(outs),
        scratch_shapes=[
            pltpu.VMEM((2, rows.shape[0], width), jnp.float32),
            pltpu.VMEM((2, taps.shape[0], 8, width), jnp.float32),
            pltpu.VMEM((n_blocks, tok_rows, width) if norm else (1, 8, width), jnp.float32),
        ],
        compiler_params=pltpu.CompilerParams(vmem_limit_bytes=VMEM_LIMIT),
        cost_estimate=pl.CostEstimate(flops=flops, bytes_accessed=rows.size * 2, transcendentals=0),
        name="conv_norm" if norm else "conv_blocks",
    )(index, taps, bias, *((gain, shift) if norm else ()), *(near(a) for a in (rows, *pieces, *done)))


def out_kernel(counts, first, index_ref, rows_ref, *refs):
    n_pieces = sum(counts)
    pieces = refs[:n_pieces]
    out, held, sems = refs[-3:]
    begin = 0
    copies = []
    for k, count in enumerate(counts):
        total = None
        at = 0
        for piece in pieces[begin : begin + count]:
            depth, width = piece.shape
            part = jnp.dot(rows_ref[:, at : at + depth], piece[...], preferred_element_type=jnp.float32)
            total = part if total is None else total + part
            at += depth
        begin += count
        held[k] = total.astype(jnp.bfloat16)
        lane = pl.multiple_of(index_ref[first + k] * width, width)
        copies.append(pltpu.make_async_copy(held.at[k], out.at[:, pl.ds(lane, width)], sems.at[k]))
        copies[-1].start()
    for copy in copies:
        copy.wait()


def out_blocks(rows, blocks, index, first, n_blocks, base=None):
    width = blocks[0][0].shape[1]
    counts = tuple(len(b) for b in blocks)
    pieces = [p for b in blocks for p in b]
    more = [] if base is None else [base]
    return pl.pallas_call(
        functools.partial(out_kernel, counts, first),
        out_shape=jax.ShapeDtypeStruct((rows.shape[0], width * n_blocks), jnp.bfloat16),
        in_specs=[whole(pltpu.SMEM)] + [whole()] * (1 + len(pieces)) + [whole(pl.ANY)] * len(more),
        out_specs=whole(pl.ANY),
        scratch_shapes=[
            pltpu.VMEM((len(blocks), rows.shape[0], width), jnp.bfloat16),
            pltpu.SemaphoreType.DMA((len(blocks),)),
        ],
        input_output_aliases={2 + len(pieces): 0} if more else {},
        compiler_params=pltpu.CompilerParams(vmem_limit_bytes=VMEM_LIMIT),
        cost_estimate=pl.CostEstimate(flops=2 * rows.size * width * len(blocks), bytes_accessed=rows.size * 6, transcendentals=0),
        name="out_blocks",
    )(index, *(near(a) for a in (rows, *pieces)), *more)


def work(activations, value_weight, gate_weight, conv_taps, conv_bias, norm_gain, norm_bias, out_weight):
    tokens = activations[0]
    n_sp, n_dp = lax.axis_size("sp"), lax.axis_size("dp")
    me = lax.axis_index("dp")

    def from_next(a):
        return lax.ppermute(a, "dp", [(i, (i - 2) % n_dp) for i in range(n_dp)])

    def from_last(a):
        return lax.ppermute(a, "dp", [(i, (i + 2) % n_dp) for i in range(n_dp)])

    def from_core(a):
        return lax.ppermute(a, "dp", [(i, i ^ 1) for i in range(n_dp)])

    halo = lax.ppermute(tokens[-HALO:], "sp", [(i, i + 1) for i in range(n_sp - 1)])

    hold = lax.optimization_barrier
    depth = value_weight.shape[0]
    packed = jnp.concatenate([jnp.concatenate([value_weight, gate_weight], axis=1), out_weight], axis=0)
    packed = (packed.astype(jnp.float32) * SCALE).astype(jnp.float16)
    packed = lax.all_gather(packed, "sp", axis=0)
    packed = (packed.astype(jnp.float32) * (1.0 / SCALE)).astype(jnp.bfloat16)
    width = packed.shape[-1]
    upper = packed[: n_sp // 2, :depth].reshape(-1, width)
    lower = packed[n_sp // 2 :, :depth].reshape(-1, width)
    o_own = packed[:, depth:].reshape(-1, width)
    o_half = o_own.shape[0] // 2
    bias, gain, shift = conv_bias[None, :], norm_gain[None, :], norm_bias[None, :]
    place = jnp.arange(n_dp, dtype=jnp.int32)
    chip = place // 2
    step = jnp.where(chip == 2, -2, jnp.where(chip == 3, 4, 2 * chip))
    index = ((me + step) % n_dp) ^ (place % 2)

    next_a, last_b = from_next(upper), from_last(lower)
    next_b, last_a = from_next(lower), from_last(upper)
    rows = jnp.concatenate([halo, tokens], axis=0)
    own_swap = [from_core(upper), from_core(lower)]
    conv_a = conv_blocks(rows, [[upper, lower], own_swap], index, 0, conv_taps, bias)
    next_a, last_b, conv_a = hold((next_a, last_b, conv_a))
    far_a, far_b = from_next(next_a), from_last(last_b)
    next_b, last_a, o_send = hold((next_b, last_a, o_own))
    o_next, o_last = from_next(o_send), from_last(o_send)
    o_swap = from_core(o_send)
    swaps = [[from_core(next_a), from_core(next_b)], [from_core(last_a), from_core(last_b)]]
    conv_b = conv_blocks(
        rows, [[next_a, next_b], swaps[0], [last_a, last_b], swaps[1]], index, 2, conv_taps, bias
    )
    far_a, far_b, conv_b = hold((far_a, far_b, conv_b))
    (swished,) = conv_blocks(
        rows, [[far_a, far_b], [from_core(far_a), from_core(far_b)]], index, 6, conv_taps, bias,
        conv_a + conv_b, gain, shift,
    )
    o_next, o_last, swished = hold((o_next, o_last, swished))
    o_far_a, o_far_b = from_next(o_next[:o_half]), from_last(o_last[o_half:])
    o_swaps = from_core(o_next), from_core(o_last)
    result = out_blocks(
        swished, [[o_send], [o_swap], [o_next], [o_swaps[0]], [o_last], [o_swaps[1]]], index, 0, n_dp
    )
    o_far_a, o_far_b, result = hold((o_far_a, o_far_b, result))
    result = out_blocks(
        swished, [[o_far_a, o_far_b], [from_core(o_far_a), from_core(o_far_b)]], index, 6, n_dp, result
    )
    return result[None]


def solution(mesh):
    in_specs = (
        P(("grp", "dp"), "sp", None),
        P("sp", "dp"),
        P("sp", "dp"),
        P(),
        P(),
        P(),
        P(),
        P("sp", "dp"),
    )
    out_specs = P(("grp", "dp"), "sp", None)
    return jax.shard_map(work, mesh=mesh, in_specs=in_specs, out_specs=out_specs, check_vma=False)
```

```python
import functools

import jax
import jax.numpy as jnp
from jax import lax
from jax.experimental import pallas as pl
from jax.experimental.pallas import tpu as pltpu
from jax.sharding import PartitionSpec as P


epsilon = 1e-05
SCALE = 2.0**18
HALO = 32
ROWS = 64
VMEM_LIMIT = 16 * 2**20


def whole(space=pltpu.VMEM):
    return pl.BlockSpec(memory_space=space)


def near(a):
    return pltpu.with_memory_space_constraint(a, pltpu.VMEM)


def convolve(gated, taps, bias, store, tok_rows):
    kernel_len = taps.shape[0]
    lead = HALO - kernel_len + 1
    for start in range(0, tok_rows, ROWS):
        n_tiles = ROWS // 8
        totals = [bias] * n_tiles
        for shift in range(8):
            near = [(q, 8 * q + shift - lead) for q in range((HALO + 8) // 8)]
            near = [(q, j) for q, j in near if 0 <= j < kernel_len]
            weights = [(q, taps[j]) for q, j in near]
            for m in range(n_tiles + near[-1][0]):
                users = [(m - q, w) for q, w in weights if 0 <= m - q < n_tiles]
                if not users:
                    continue
                row = gated[pl.ds(start + 8 * m + shift, 8), :]
                for tile, w in users:
                    totals[tile] = totals[tile] + w * row
        for tile, total in enumerate(totals):
            store(start + 8 * tile, total)


def conv_kernel(counts, first, n_done, index_ref, taps_ref, bias_ref, *refs):
    n_pieces, n_blocks = sum(counts), len(counts)
    norm = n_done > 0
    if norm:
        (gain_ref, shift_ref), refs = refs[:2], refs[2:]
    rows, pieces, refs = refs[0], refs[1 : 1 + n_pieces], refs[1 + n_pieces :]
    done, refs = refs[:n_done], refs[n_done:]
    n_outs = 1 if norm else n_blocks
    outs, refs = refs[:n_outs], refs[n_outs:]
    gated, taps_held, conv = refs
    tok_rows, width = rows.shape[0] - HALO, gated.shape[-1]
    kernel_len = taps_ref.shape[0]

    def lane_of(k):
        return pl.multiple_of(index_ref[first + k] * width, width)

    def project(k):
        at, total = 0, None
        for piece in pieces[sum(counts[:k]) : sum(counts[: k + 1])]:
            size = piece.shape[0]
            part = jnp.dot(rows[:, at : at + size], piece[...], preferred_element_type=jnp.float32)
            total = part if total is None else total + part
            at += size
        return total

    def gate(k, both):
        value = both[:, :width].astype(jnp.bfloat16).astype(jnp.float32)
        gates = both[:, width:].astype(jnp.bfloat16).astype(jnp.float32)
        gated[k % 2] = (value * jax.nn.sigmoid(gates)).astype(jnp.bfloat16).astype(jnp.float32)
        for j in range(kernel_len):
            taps_held[k % 2, j] = jnp.broadcast_to(taps_ref[j : j + 1, pl.ds(lane_of(k), width)], (8, width))

    def filter_block(k):
        bias = jnp.broadcast_to(bias_ref[:, pl.ds(lane_of(k), width)], (8, width))

        def store(at, value):
            if norm:
                conv[k, pl.ds(at, 8), :] = value
            else:
                outs[k][pl.ds(at, 8), :] = value

        convolve(gated.at[k % 2], taps_held.at[k % 2], bias, store, tok_rows)

    gate(0, project(0))
    for k in range(1, n_blocks):
        both = project(k)
        filter_block(k - 1)
        gate(k, both)
    filter_block(n_blocks - 1)
    if not norm:
        return

    out = outs[0]
    total = n_done + n_blocks
    lanes = [pl.multiple_of(index_ref[k] * width, width) for k in range(total)]

    def tile(i, carry):
        at = pl.ds(pl.multiple_of(i * 16, 16), 16)
        values = [d[at, :] for d in done] + [conv[k, at, :] for k in range(n_blocks)]
        mean = jnp.sum(sum(values[1:], values[0]), axis=-1, keepdims=True) / (total * width)
        values = [v - mean for v in values]
        squares = [v * v for v in values]
        spread = jnp.sum(sum(squares[1:], squares[0]), axis=-1, keepdims=True) / (total * width)
        scale = lax.rsqrt(spread + epsilon)
        for v, lane in zip(values, lanes):
            normed = v * scale * gain_ref[:, pl.ds(lane, width)] + shift_ref[:, pl.ds(lane, width)]
            out[at, pl.ds(lane, width)] = jax.nn.silu(normed).astype(jnp.bfloat16)
        return carry

    lax.fori_loop(0, tok_rows // 16, tile, 0, unroll=4)


def conv_blocks(rows, blocks, index, first, taps, bias, done=(), gain=None, shift=None):
    tok_rows = rows.shape[0] - HALO
    width = blocks[0][0].shape[1] // 2
    counts = tuple(len(b) for b in blocks)
    pieces = [p for b in blocks for p in b]
    n_blocks, n_done = len(blocks), len(done)
    norm = n_done > 0
    if norm:
        outs = [pltpu.VMEM((tok_rows, width * (n_done + n_blocks)), jnp.bfloat16)]
    else:
        outs = [pltpu.VMEM((tok_rows, width), jnp.float32) for _ in blocks]
    flops = 2 * rows.shape[0] * rows.shape[1] * 2 * width * n_blocks
    return pl.pallas_call(
        functools.partial(conv_kernel, counts, first, n_done),
        out_shape=outs,
        in_specs=[whole(pltpu.SMEM)]
        + [whole()] * (4 if norm else 2)
        + [whole()] * (1 + len(pieces) + n_done),
        out_specs=[whole()] * len(outs),
        scratch_shapes=[
            pltpu.VMEM((2, rows.shape[0], width), jnp.float32),
            pltpu.VMEM((2, taps.shape[0], 8, width), jnp.float32),
            pltpu.VMEM((n_blocks, tok_rows, width) if norm else (1, 8, width), jnp.float32),
        ],
        compiler_params=pltpu.CompilerParams(vmem_limit_bytes=VMEM_LIMIT),
        cost_estimate=pl.CostEstimate(flops=flops, bytes_accessed=rows.size * 2, transcendentals=0),
        name="conv_norm" if norm else "conv_blocks",
    )(index, taps, bias, *((gain, shift) if norm else ()), *(near(a) for a in (rows, *pieces, *done)))


def out_kernel(counts, first, index_ref, rows_ref, *refs):
    n_pieces = sum(counts)
    pieces = refs[:n_pieces]
    out, held, sems = refs[-3:]
    begin = 0
    copies = []
    for k, count in enumerate(counts):
        total = None
        at = 0
        for piece in pieces[begin : begin + count]:
            depth, width = piece.shape
            part = jnp.dot(rows_ref[:, at : at + depth], piece[...], preferred_element_type=jnp.float32)
            total = part if total is None else total + part
            at += depth
        begin += count
        held[k] = total.astype(jnp.bfloat16)
        lane = pl.multiple_of(index_ref[first + k] * width, width)
        copies.append(pltpu.make_async_copy(held.at[k], out.at[:, pl.ds(lane, width)], sems.at[k]))
        copies[-1].start()
    for copy in copies:
        copy.wait()


def out_blocks(rows, blocks, index, first, n_blocks, base=None):
    width = blocks[0][0].shape[1]
    counts = tuple(len(b) for b in blocks)
    pieces = [p for b in blocks for p in b]
    more = [] if base is None else [base]
    return pl.pallas_call(
        functools.partial(out_kernel, counts, first),
        out_shape=jax.ShapeDtypeStruct((rows.shape[0], width * n_blocks), jnp.bfloat16),
        in_specs=[whole(pltpu.SMEM)] + [whole()] * (1 + len(pieces)) + [whole(pl.ANY)] * len(more),
        out_specs=whole(pl.ANY),
        scratch_shapes=[
            pltpu.VMEM((len(blocks), rows.shape[0], width), jnp.bfloat16),
            pltpu.SemaphoreType.DMA((len(blocks),)),
        ],
        input_output_aliases={2 + len(pieces): 0} if more else {},
        compiler_params=pltpu.CompilerParams(vmem_limit_bytes=VMEM_LIMIT),
        cost_estimate=pl.CostEstimate(flops=2 * rows.size * width * len(blocks), bytes_accessed=rows.size * 6, transcendentals=0),
        name="out_blocks",
    )(index, *(near(a) for a in (rows, *pieces)), *more)


def work(activations, value_weight, gate_weight, conv_taps, conv_bias, norm_gain, norm_bias, out_weight):
    tokens = activations[0]
    n_sp, n_dp = lax.axis_size("sp"), lax.axis_size("dp")
    me = lax.axis_index("dp")

    def from_next(a):
        return lax.ppermute(a, "dp", [(i, (i - 2) % n_dp) for i in range(n_dp)])

    def from_last(a):
        return lax.ppermute(a, "dp", [(i, (i + 2) % n_dp) for i in range(n_dp)])

    def from_core(a):
        return lax.ppermute(a, "dp", [(i, i ^ 1) for i in range(n_dp)])

    halo = lax.ppermute(tokens[-HALO:], "sp", [(i, i + 1) for i in range(n_sp - 1)])

    hold = lax.optimization_barrier
    depth = value_weight.shape[0]
    packed = jnp.concatenate([jnp.concatenate([value_weight, gate_weight], axis=1), out_weight], axis=0)
    packed = (packed.astype(jnp.float32) * SCALE).astype(jnp.float16)
    packed = lax.all_gather(packed, "sp", axis=0)
    packed = (packed.astype(jnp.float32) * (1.0 / SCALE)).astype(jnp.bfloat16)
    width = packed.shape[-1]
    upper = packed[: n_sp // 2, :depth].reshape(-1, width)
    lower = packed[n_sp // 2 :, :depth].reshape(-1, width)
    o_own = packed[:, depth:].reshape(-1, width)
    upper, lower, o_own = hold((upper, lower, o_own))
    o_half = o_own.shape[0] // 2
    bias, gain, shift = conv_bias[None, :], norm_gain[None, :], norm_bias[None, :]
    n_grp = lax.axis_size("grp")
    sign = 1 - 2 * (lax.axis_index("grp") % 2)
    place = jnp.arange(n_dp, dtype=jnp.int32)
    chip = place // 2
    v_step = jnp.where(chip == 1, 4, jnp.where(chip == 2, 2, jnp.where(chip == 3, -2, 0)) * sign)
    o_step = jnp.where(chip == 2, -2, jnp.where(chip == 3, 4, 2 * chip))
    v_index = ((me + v_step) % n_dp) ^ (place % 2)
    o_index = ((me + o_step) % n_dp) ^ (place % 2)

    def along(step, a):
        pairs = []
        for g in range(n_grp):
            away = step if g % 2 == 0 else -step
            pairs += [(g * n_dp + i, g * n_dp + (i - away) % n_dp) for i in range(n_dp)]
        return lax.ppermute(a, ("grp", "dp"), pairs)

    def from_group(a):
        return lax.ppermute(a, "grp", [(g, g ^ 1) for g in range(n_grp)])

    near_a, near_b = along(2, upper), along(-2, lower)
    rows = jnp.concatenate([halo, tokens], axis=0)
    own_swap = [from_core(upper), from_core(lower)]
    far_a, far_b = along(2, near_a), along(-2, near_b)
    pair_a, pair_b = from_group(near_a), from_group(near_b)
    o_next, o_last = from_next(o_own), from_last(o_own)
    conv_a = conv_blocks(rows, [[upper, lower], own_swap], v_index, 0, conv_taps, bias)
    near_a, near_b, far_a, far_b, conv_a, o_own = hold((near_a, near_b, far_a, far_b, conv_a, o_own))
    near_swap_a, near_swap_b = from_core(near_a), from_core(near_b)
    o_swap = from_core(o_own)
    conv_b = conv_blocks(
        rows, [[far_a, far_b], [from_core(far_a), from_core(far_b)]], v_index, 2, conv_taps, bias
    )
    o_next, o_last, conv_b = hold((o_next, o_last, conv_b))
    o_far_a, o_far_b = from_next(o_next[:o_half]), from_last(o_last[o_half:])
    o_swaps = from_core(o_next), from_core(o_last)
    pair_swap_a, pair_swap_b = from_core(pair_a), from_core(pair_b)
    (swished,) = conv_blocks(
        rows,
        [[near_a, pair_b], [near_swap_a, pair_swap_b], [pair_a, near_b], [pair_swap_a, near_swap_b]],
        v_index, 4, conv_taps, bias, conv_a + conv_b, gain, shift,
    )
    o_far_a, o_far_b, swished = hold((o_far_a, o_far_b, swished))
    o_far_swap = from_core(o_far_a), from_core(o_far_b)
    result = out_blocks(swished, [[o_own], [o_swap], [o_next], [o_swaps[0]], [o_last], [o_swaps[1]]], o_index, 0, n_dp)
    result = out_blocks(swished, [[o_far_a, o_far_b], list(o_far_swap)], o_index, 6, n_dp, result)
    return result[None]


def solution(mesh):
    in_specs = (
        P(("grp", "dp"), "sp", None),
        P("sp", "dp"),
        P("sp", "dp"),
        P(),
        P(),
        P(),
        P(),
        P("sp", "dp"),
    )
    out_specs = P(("grp", "dp"), "sp", None)
    return jax.shard_map(work, mesh=mesh, in_specs=in_specs, out_specs=out_specs, check_vma=False)
```
